32 devices in a mesh: ep: 8 (over z, x), tp: 4 (over y, core).
Axes of the slice: x: 2, y: 2, z: 4, core: 2. Of those that a mesh axis runs over, the one named last changes fastest.
Arguments:
- tokens: bfloat16 [192, 2048], P('ep'), may hold values from -12 to 12
- state: float32 [192, 16, 128, 256], P('ep', 'tp'), may hold values from -6 to 6
- w_query: bfloat16 [2048, 2048], P(None, 'tp'), may hold values from -0.125 to 0.125
- w_key: bfloat16 [2048, 2048], P(None, 'tp'), may hold values from -0.125 to 0.125
- w_value: bfloat16 [2048, 4096], P(None, 'tp'), may hold values from -0.125 to 0.125
- w_outgate: bfloat16 [2048, 4096], P(None, 'tp'), may hold values from -0.125 to 0.125
- decay_down: bfloat16 [2048, 16], replicated, may hold values from -0.125 to 0.125
- decay_up: bfloat16 [16, 2048], P(None, 'tp'), may hold values from -9 to 9
- decay_bias: float32 [2048], P('tp'), may hold values from -6 to 4
- head_gain: float32 [256], replicated, may hold values from 0.1 to 1.9
- w_output: bfloat16 [4096, 2048], P('tp'), may hold values from -0.09375 to 0.09375
- norm1_gain: float32 [2048], P('tp'), may hold values from 0.1 to 1.9
- route_ids: int32 [192, 6], P('ep'), may hold values from 0 to 31, all different within a row; in each aligned block of 24 rows (0 to 23, 24 to 47, ...) at most 5 rows name the same one
- route_weight: float32 [192, 6], P('ep'), may hold values from 0.1 to 1
- exp_gate: bfloat16 [32, 2048, 512], P('ep', 'tp'), may hold values from -0.125 to 0.125
- exp_up: bfloat16 [32, 2048, 512], P('ep', 'tp'), may hold values from -0.125 to 0.125
- exp_down: bfloat16 [32, 512, 2048], P('ep', None, 'tp'), may hold values from -0.25 to 0.25
- sh_gate: bfloat16 [2048, 512], P('tp'), may hold values from -0.125 to 0.125
- sh_up: bfloat16 [2048, 512], P('tp'), may hold values from -0.125 to 0.125
- sh_down: bfloat16 [512, 2048], P(None, 'tp'), may hold values from -0.25 to 0.25
- norm2_gain: float32 [2048], P('tp'), may hold values from 0.1 to 1.9
Outputs:
- layer_out: bfloat16 [192, 2048], P('ep', 'tp')
The draws below stay inside these ranges and needn't reach their ends.
Inputs may be any that keep to these rules, and one draw needn't show every extreme that they name: `route_ids`: each row names 6 different experts. Among the rows of one index of ep (aligned blocks of 24 rows) no expert is named by more than 5 rows, and in some blocks one expert is named by exactly 5.
All inputs are finite; a program needn't handle non-finite values.
Results may differ from the reference program's by a relative error of at most 0.02.
Values may be sent and summed in bfloat16 or wider, within the bound.
A program may use at most 64 MiB of HBM per device.

```python
import math
import jax
import jax.numpy as jnp
import numpy as np
from jax import lax

D = 2048
HEADS = 16
KEY_DIM = 128
VAL_DIM = 256
RANK = 16
FF_EXP = 512
FF_SHARED = 512
TOPK = 6
TOK_DEV = 24
BATCH = 192
EXPERTS = 32
CAP = 5
N_EP = 8
N_TP = 4


def draw_tokens(key, part):
    column = jnp.arange(D, dtype=jnp.float32) / D
    ramp = jnp.exp((2.0 * column - 1.0) * jnp.log(3.0))
    drawn = jax.random.normal(key, (BATCH, D), jnp.float32) * ramp
    return jnp.clip(drawn, -12.0, 12.0).astype(jnp.bfloat16)


def block_scale(stream_key, dims, cuts, smallest, top_value):
    loudness, own = 1.0, jax.random.fold_in(stream_key, 6)
    for axis_at, shards_of in cuts:
        heights = jnp.exp(jax.random.uniform(jax.random.fold_in(own, axis_at), (shards_of,), jnp.float32, smallest / len(cuts), top_value / len(cuts)))
        loudness = loudness * jnp.repeat(heights, dims[axis_at] // shards_of).reshape([-1 if axis == axis_at else 1 for axis in range(len(dims))])
    return loudness


def assign_block(rng, own, number, rows, number_of, top, limit, lean):
    sequence = jax.random.permutation(rng, number_of)
    heavy_load, common = load_shares(number_of, rows * top, limit, lean, True), load_shares(number_of, rows * top, limit, lean, False)
    places = jnp.arange(number_of)

    def named(lengths, turn):
        used = int((lengths > 0).sum())
        fixed = max(1, used // 4)
        moved = fixed + (places - fixed + turn * (used - fixed)) % max(1, number_of - fixed)
        return jnp.zeros((number_of,), jnp.int32).at[sequence[jnp.where(places < fixed, places, moved)]].set(jnp.asarray(lengths, jnp.int32))

    lengths = jnp.where(number % 4 == 0, named(heavy_load, number // 4), named(common, number - number // 4 - 1))
    mixed = jax.random.permutation(jax.random.fold_in(own, 3), number_of)
    giver, sink = mixed[0:number_of // 2 * 2:2], mixed[1:number_of // 2 * 2:2]
    margin = jnp.minimum(lengths[giver] - 1, limit - lengths[sink]) // 2
    margin = jnp.where((giver == sequence[0]) | (sink == sequence[0]) | (lengths[sink] == 0), 0, jnp.maximum(margin, 0))
    moved = jax.random.randint(jax.random.fold_in(own, 4), (number_of // 2,), 0, 1 << 20) % (margin + 1)
    lengths = lengths.at[giver].add(-moved).at[sink].add(moved)
    members = jnp.searchsorted(jnp.cumsum(lengths), jnp.arange(rows * top), side="right").astype(jnp.int32)
    listing = members.reshape(top, rows).T
    listing = listing[jax.random.permutation(jax.random.fold_in(own, 1), rows)]
    turn = jax.random.randint(jax.random.fold_in(own, 2), (rows, 1), 0, top)
    return jnp.take_along_axis(listing, (jnp.arange(top)[None, :] + turn) % top, axis=1)


def load_shares(count, total, reach, skew, full):
    weights = [(1 << 20) // math.isqrt(grade ** skew) + 1 for grade in range(1, count + 1)]
    largest = reach if full else min(reach, max(-(-total // count), total * weights[0] // sum(weights)))
    least = 1 if total - largest >= count - 1 else 0
    holding, spare = [largest] + [least] * (count - 1), total - largest - least * (count - 1)
    while spare > 0:
        movable = [i for i in range(1, count) if holding[i] < largest] or [i for i in range(1, count) if holding[i] < reach]
        whole, remaining = sum([weights[i] for i in movable]), spare
        for i in movable:
            more = min(reach - holding[i], max(1, remaining * weights[i] // whole), spare)
            holding[i] = holding[i] + more
            spare = spare - more
    return np.array(holding)


def noise(stream_key, extent, scale, limit, cuts=(), kind=jnp.bfloat16):
    loudness = block_scale(stream_key, extent, cuts, -0.22, 0.18) if cuts else 1.0
    values = jax.random.normal(stream_key, extent, jnp.float32) * scale * loudness
    return jnp.minimum(jnp.maximum(values, -limit), limit).astype(kind)


def setup_inputs(seed: int = 0) -> dict:
    keys = jax.random.split(jax.random.key(seed), 22)
    tokens = draw_tokens(jax.random.fold_in(keys[21], 71), 0)
    state = noise(keys[1], (BATCH, HEADS, KEY_DIM, VAL_DIM), 1.0, 6.0, ((0, 8), (1, 4)), jnp.float32)
    w_query = noise(keys[2], (D, HEADS * KEY_DIM), D ** -0.5, 0.125, ((1, 4),))
    w_key = noise(keys[3], (D, HEADS * KEY_DIM), D ** -0.5, 0.125, ((1, 4),))
    w_value = noise(keys[4], (D, HEADS * VAL_DIM), D ** -0.5, 0.125, ((1, 4),))
    w_outgate = noise(keys[5], (D, HEADS * VAL_DIM), D ** -0.5, 0.125, ((1, 4),))
    decay_down = noise(keys[6], (D, RANK), D ** -0.5, 0.125)
    decay_up = noise(keys[7], (RANK, HEADS * KEY_DIM), 1.5, 9.0, ((1, 4),))
    decay_bias = jnp.clip(-6.0 + 10.0 * jax.random.uniform(keys[8], (HEADS * KEY_DIM,), jnp.float32) ** block_scale(keys[8], (HEADS * KEY_DIM,), ((0, 4),), -0.2, 0.2), -6.0, 4.0)
    head_gain = jnp.clip(1.0 + 0.18 * jax.random.normal(keys[9], (VAL_DIM,), jnp.float32), 0.1, 1.9)
    w_output = noise(keys[10], (HEADS * VAL_DIM, D), (HEADS * VAL_DIM) ** -0.5, 0.09375, ((0, 4),))
    norm1_gain = jnp.clip(1.0 + 0.18 * jax.random.normal(keys[11], (D,), jnp.float32), 0.1, 1.9)
    route_ids_keys = jax.random.split(jax.random.fold_in(keys[12], 1), BATCH // TOK_DEV)
    route_ids_turns = jax.random.permutation(jax.random.fold_in(keys[12], 3), BATCH // TOK_DEV)
    route_ids = jax.vmap(lambda own, number: assign_block(jax.random.fold_in(keys[12], 2), own, number, TOK_DEV, EXPERTS, TOPK, CAP, 2))(route_ids_keys, route_ids_turns).reshape((BATCH, TOPK))
    route_weight = jnp.clip(0.1 + 0.9 * jax.random.uniform(keys[13], (BATCH, TOPK), jnp.float32) ** block_scale(keys[13], (BATCH, TOPK), ((0, 8),), -0.2, 0.2), 0.1, 1.0)
    exp_gate = noise(keys[14], (EXPERTS, D, FF_EXP), D ** -0.5, 0.125, ((0, 8), (1, 4)))
    exp_up = noise(keys[15], (EXPERTS, D, FF_EXP), D ** -0.5, 0.125, ((0, 8), (1, 4)))
    exp_down = noise(keys[16], (EXPERTS, FF_EXP, D), FF_EXP ** -0.5, 0.25, ((0, 8), (2, 4)))
    sh_gate = noise(keys[17], (D, FF_SHARED), D ** -0.5, 0.125, ((0, 4),))
    sh_up = noise(keys[18], (D, FF_SHARED), D ** -0.5, 0.125, ((0, 4),))
    sh_down = noise(keys[19], (FF_SHARED, D), FF_SHARED ** -0.5, 0.25, ((1, 4),))
    norm2_gain = jnp.clip(1.0 + 0.18 * jax.random.normal(keys[20], (D,), jnp.float32), 0.1, 1.9)
    return dict(tokens=tokens, state=state, w_query=w_query, w_key=w_key, w_value=w_value, w_outgate=w_outgate, decay_down=decay_down, decay_up=decay_up, decay_bias=decay_bias, head_gain=head_gain, w_output=w_output, norm1_gain=norm1_gain, route_ids=route_ids, route_weight=route_weight, exp_gate=exp_gate, exp_up=exp_up, exp_down=exp_down, sh_gate=sh_gate, sh_up=sh_up, sh_down=sh_down, norm2_gain=norm2_gain)


res_scale = 2.0 ** 0.5
decay_tau = 16.0
norm_eps = 1e-05

def settle(values):
    return lax.optimization_barrier(values.astype(jnp.bfloat16)).astype(jnp.float32)

def project(left, right):
    return jnp.dot(left, right, preferred_element_type=jnp.float32)

def grouped_sum(left, right, group_count):
    width = right.shape[0] // group_count

    def add_group(running, group_index):
        left_piece = lax.dynamic_slice_in_dim(left, group_index * width, width, 1)
        right_block = lax.dynamic_slice_in_dim(right, group_index * width, width, 0)
        return (running + settle(project(left_piece, right_block)), None)
    start = jnp.zeros((left.shape[0], right.shape[1]), jnp.float32)
    running, _ = lax.scan(add_group, start, jnp.arange(group_count, dtype=jnp.int32))
    return running

def layer_norm(values, gain):
    center = values - lax.optimization_barrier(jnp.mean(values, -1, keepdims=True))
    spread = lax.optimization_barrier(jnp.mean(center * center, -1, keepdims=True))
    return center * lax.rsqrt(spread + norm_eps) * gain

def reference(tokens, state, w_query, w_key, w_value, w_outgate, decay_down, decay_up, decay_bias, head_gain, w_output, norm1_gain, route_ids, route_weight, exp_gate, exp_up, exp_down, sh_gate, sh_up, sh_down, norm2_gain):
    queries = settle(project(tokens, w_query)).reshape(BATCH, HEADS, KEY_DIM) * KEY_DIM ** (-0.5)
    key_rows = settle(project(tokens, w_key)).reshape(BATCH, HEADS, KEY_DIM)
    values = settle(project(tokens, w_value)).reshape(BATCH, HEADS, VAL_DIM)
    gate_pre = settle(project(tokens, w_outgate)).reshape(BATCH, HEADS, VAL_DIM)
    decay_low = lax.optimization_barrier(project(tokens, decay_down).astype(jnp.bfloat16))
    log_decay = (jax.nn.log_sigmoid(project(decay_low, decay_up) + decay_bias) / decay_tau).reshape(BATCH, HEADS, KEY_DIM)
    carried = jnp.einsum('bhk,bhkv->bhv', queries * jnp.exp(log_decay), state, precision=lax.Precision.HIGHEST)
    attended = carried + lax.optimization_barrier(jnp.sum(queries * key_rows, -1, keepdims=True)) * values
    inv_norm = lax.rsqrt(lax.optimization_barrier(jnp.mean(attended * attended, -1, keepdims=True)) + norm_eps)
    head_out = (attended * inv_norm * head_gain * jax.nn.silu(gate_pre)).astype(jnp.bfloat16).reshape(BATCH, HEADS * VAL_DIM)
    mixed = settle(grouped_sum(head_out, w_output, N_TP))
    normed_mid = layer_norm(res_scale * tokens.astype(jnp.float32) + mixed, norm1_gain)
    normed_mid = lax.optimization_barrier(normed_mid.astype(jnp.bfloat16))
    pair_count = TOK_DEV * TOPK
    expert_ids = route_ids.reshape(N_EP, pair_count)
    onehot = (expert_ids[:, :, None] == jnp.arange(EXPERTS, dtype=jnp.int32)[None, None, :]).astype(jnp.int32)
    ranks = lax.optimization_barrier(jnp.sum((jnp.cumsum(onehot, 1) - 1) * onehot, -1))
    group_ids = jnp.arange(N_EP, dtype=jnp.int32)[:, None]
    positions = (expert_ids * (N_EP * CAP) + group_ids * CAP + ranks).reshape(BATCH * TOPK)
    token_ids = jnp.arange(BATCH * TOPK, dtype=jnp.int32) // TOPK
    table = jnp.full((EXPERTS * N_EP * CAP,), BATCH, jnp.int32).at[positions].set(token_ids)
    padded = jnp.concatenate([normed_mid, jnp.zeros((1, D), jnp.bfloat16)], 0)

    def one_expert(operands):
        row_ids, gate_weight, up_weight, down_weight = operands
        chosen = padded[row_ids]
        gate_sum = settle(grouped_sum(chosen, gate_weight, N_TP))
        up_sum = settle(grouped_sum(chosen, up_weight, N_TP))
        inner = (jax.nn.silu(gate_sum) * up_sum).astype(jnp.bfloat16)
        return project(inner, down_weight).astype(jnp.bfloat16)
    expert_out = lax.map(one_expert, (table.reshape(EXPERTS, N_EP * CAP), exp_gate, exp_up, exp_down))
    expert_out = expert_out.reshape(EXPERTS * N_EP * CAP, D)
    picked = expert_out[positions].astype(jnp.float32).reshape(BATCH, TOPK, D)
    routed = lax.optimization_barrier(jnp.sum(picked * route_weight[:, :, None], 1))
    shared_gate = settle(grouped_sum(normed_mid, sh_gate, N_TP))
    shared_up = settle(grouped_sum(normed_mid, sh_up, N_TP))
    shared_inner = (jax.nn.silu(shared_gate) * shared_up).astype(jnp.bfloat16)
    mixture = routed + project(shared_inner, sh_down)
    return layer_norm(res_scale * normed_mid.astype(jnp.float32) + mixture, norm2_gain).astype(jnp.bfloat16)
```

```python
import functools

import jax
import jax.numpy as jnp
from jax import lax
from jax.experimental import pallas as pl
from jax.experimental.pallas import tpu as pltpu
from jax.sharding import PartitionSpec as P

res_scale = 2.0**0.5
decay_tau = 16.0
norm_eps = 1e-05
AHEAD = 6
F32 = jnp.float32
BF16 = jnp.bfloat16


def dot(left, right):
    return jnp.dot(left, right, preferred_element_type=F32)


def dot_nt(left, right):
    return lax.dot_general(left, right, (((1,), (1,)), ((), ())), preferred_element_type=F32)


def iota_f(shape, dim):
    return lax.broadcasted_iota(jnp.int32, shape, dim).astype(F32)


def quotient(values, divisor):
    return jnp.floor((values + 0.5) * (1.0 / divisor))


def silu(x):
    return x * (1.0 / (1.0 + jnp.exp(-x)))


def kernel(
    dims,
    tokens,
    decay_down,
    decay_up,
    decay_bias,
    head_gain,
    norm1_gain,
    route_ids,
    route_weight,
    norm2_gain,
    state_h,
    wq_h,
    wk_h,
    wv_h,
    wg_h,
    wo_h,
    eg_h,
    eu_h,
    ed_h,
    sg_h,
    su_h,
    sd_h,
    out,
    state,
    wq,
    wk,
    wv,
    wg,
    wo,
    eg,
    eu,
    ed,
    sg,
    su,
    sd,
    dq_ref,
    att_ref,
    head_out,
    p1s,
    p1r,
    p2s,
    p2r,
    p3s,
    p3r,
    p4s,
    p4r,
    p4hs,
    p4hr,
    p5,
    p5h,
    p6s,
    p6r,
    p7s,
    p7r,
    load_sem,
    tp_send,
    tp_recv,
    ep_send,
    ep_recv,
):
    (rows, heads, kdim, vdim, cols, tp, ep, local, cap, rd, groups, fc, fsc, top, chunks) = dims
    experts = local * ep
    slots = ep * rd
    me_t = lax.axis_index("tp")
    me_e = lax.axis_index("ep")

    def tp_peer(offset):
        return lax.rem(me_t + offset, tp)

    def ep_peer(offset):
        return lax.rem(me_e + offset, ep)

    barrier = pltpu.get_barrier_semaphore()
    for offset in range(1, tp):
        pl.semaphore_signal(
            barrier, inc=1, device_id=(me_e, tp_peer(offset)), device_id_type=pl.DeviceIdType.MESH
        )
    for offset in range(1, ep):
        pl.semaphore_signal(
            barrier, inc=1, device_id=(ep_peer(offset), me_t), device_id_type=pl.DeviceIdType.MESH
        )

    loads = []

    def add_load(src, dst):
        loads.append(pltpu.make_async_copy(src, dst, load_sem.at[len(loads)]))
        return len(loads) - 1

    step = rows // chunks
    i_wq = add_load(wq_h, wq)
    i_wk = add_load(wk_h, wk)
    i_state = [
        add_load(state_h.at[pl.ds(c * step, step)], state.at[pl.ds(c * step, step)])
        for c in range(chunks)
    ]
    half = wv_h.shape[0] // 2
    i_wv = [add_load(wv_h.at[pl.ds(c * half, half)], wv.at[pl.ds(c * half, half)]) for c in range(2)]
    i_wg = [add_load(wg_h.at[pl.ds(c * half, half)], wg.at[pl.ds(c * half, half)]) for c in range(2)]
    i_wo = []
    for offset in range(tp):
        start = pl.multiple_of(tp_peer(offset + 1) * cols, 128)
        i_wo.append(add_load(wo_h.at[:, pl.ds(start, cols)], wo.at[offset]))
    i_sg = add_load(sg_h, sg)
    i_su = add_load(su_h, su)
    i_eg = add_load(eg_h, eg)
    i_eu = add_load(eu_h, eu)
    i_sd = add_load(sd_h, sd)
    i_ed = add_load(ed_h, ed)
    for copy in loads[:AHEAD]:
        copy.start()

    def ready(index):
        loads[index].wait()
        if index + AHEAD < len(loads):
            loads[index + AHEAD].start()

    def tp_copy(src, dst, kind, slot, target):
        return pltpu.make_async_remote_copy(
            src_ref=src,
            dst_ref=dst,
            send_sem=tp_send.at[kind, slot],
            recv_sem=tp_recv.at[kind, slot],
            device_id=(me_e, target),
            device_id_type=pl.DeviceIdType.MESH,
        )

    def ep_copy(src, dst, kind, slot, target):
        return pltpu.make_async_remote_copy(
            src_ref=src,
            dst_ref=dst,
            send_sem=ep_send.at[kind, slot],
            recv_sem=ep_recv.at[kind, slot],
            device_id=(target, me_t),
            device_id_type=pl.DeviceIdType.MESH,
        )

    tok = tokens[...]
    decay_low = dot(tok, decay_down[...]).astype(BF16)
    pre = dot(decay_low, decay_up[...]) + decay_bias[...]
    log_decay = (jnp.minimum(pre, 0.0) - jnp.log(1.0 + jnp.exp(-jnp.abs(pre)))) * (1.0 / decay_tau)
    ids = route_ids[...]
    weights = route_weight[...]
    expert_iota = lax.broadcasted_iota(jnp.int32, (rows, experts), 1)
    member = jnp.zeros((rows, experts), F32)
    weight_of = jnp.zeros((rows, experts), F32)
    for k in range(top):
        hit = ids[:, k : k + 1] == expert_iota
        member = jnp.where(hit, 1.0, member)
        weight_of = jnp.where(hit, weights[:, k : k + 1], weight_of)
    member_b = member.astype(BF16)
    earlier = (iota_f((rows, rows), 1) < iota_f((rows, rows), 0)).astype(F32).astype(BF16)
    rank_b = dot(earlier, member_b).astype(BF16)

    def slot_parts(number):
        dest = quotient(number, rd)
        inner = number - dest * rd
        which = quotient(inner, cap)
        return dest * local + which, inner - which * cap, which, inner < local * cap

    e_row, c_row, _, ok_row = slot_parts(iota_f((1, slots), 1))
    expand = ((iota_f((experts, slots), 0) == e_row) & ok_row).astype(F32).astype(BF16)
    e_col, c_col, _, ok_col = slot_parts(iota_f((slots, 1), 0))
    expand_t = ((iota_f((slots, experts), 1) == e_col) & ok_col).astype(F32).astype(BF16)
    place = jnp.where(
        (dot_nt(expand_t, member_b) > 0.5) & (dot_nt(expand_t, rank_b) == c_col), 1.0, 0.0
    ).astype(BF16)
    place_t = (dot(member_b, expand) > 0.5) & (dot(rank_b, expand) == c_row)
    weight_hi = weight_of.astype(BF16)
    weight_lo = (weight_of - weight_hi.astype(F32)).astype(BF16)
    gather_hi = jnp.where(place_t, dot(weight_hi, expand), 0.0).astype(BF16)
    gather_lo = jnp.where(place_t, dot(weight_lo, expand), 0.0).astype(BF16)
    row_expert = slot_parts(iota_f((slots, 1), 0))[2]

    ready(i_wq)
    queries = dot(tok, wq[...]).astype(BF16).astype(F32) * kdim ** (-0.5)
    dq_ref[...] = queries * jnp.exp(log_decay)
    ready(i_wk)
    key_rows = dot(tok, wk[...]).astype(BF16).astype(F32)
    pairs = queries * key_rows
    width = heads * kdim
    hr = att_ref.shape[1]
    head_mask = quotient(iota_f((hr, width), 1), kdim) == iota_f((hr, width), 0)
    for c in range(chunks):
        ready(i_state[c])

        def one_row(b, carry):
            left = jnp.where(head_mask, dq_ref[pl.ds(b, 1), :], 0.0).astype(BF16)
            right = state[b].reshape(width, vdim).astype(BF16)
            att_ref[b] = dot(left, right)
            return carry

        lax.fori_loop(c * step, (c + 1) * step, one_row, 0, unroll=min(step, 3))
    for i in i_wv:
        ready(i)
    values = dot(tok, wv[...]).astype(BF16).astype(F32)
    for i in i_wg:
        ready(i)
    gate_pre = dot(tok, wg[...]).astype(BF16).astype(F32)
    for h in range(heads):
        part = slice(h * vdim, (h + 1) * vdim)
        score = jnp.sum(pairs[:, h * kdim : (h + 1) * kdim], -1, keepdims=True)
        attended = att_ref[:, h, :] + score * values[:, part]
        inv = lax.rsqrt(jnp.mean(attended * attended, -1, keepdims=True) + norm_eps)
        head_out[:, part] = (attended * inv * head_gain[...] * silu(gate_pre[:, part])).astype(BF16)
    pl.semaphore_wait(barrier, tp - 1 + ep - 1)

    sent = []
    heads_side = head_out[...]
    own = None
    for offset in range(1, tp + 1):
        ready(i_wo[offset - 1])
        product = dot(heads_side, wo[offset - 1])
        if offset < tp:
            p1s[offset] = product.astype(BF16)
            copy = tp_copy(p1s.at[offset], p1r.at[offset], 0, offset, tp_peer(offset))
            copy.start()
            sent.append(copy)
        else:
            own = product
    start = pl.multiple_of(me_t * cols, 128)
    resid = own + res_scale * tokens[:, pl.ds(start, cols)].astype(F32)
    for offset in range(1, tp):
        sent[offset - 1].wait_recv()
        resid = resid + p1r[offset].astype(F32)

    def layer_norm(values, send_ref, recv_ref, kind, gain):
        mean = jnp.mean(values, -1, keepdims=True)
        center = values - mean
        moment = jnp.sum(center * center, -1, keepdims=True)
        lane = lax.broadcasted_iota(jnp.int32, (rows, 128), 1)
        send_ref[...] = jnp.where(lane == 0, mean, moment)
        copies = []
        for offset in range(1, tp):
            copy = tp_copy(send_ref, recv_ref.at[offset], kind, offset, tp_peer(offset))
            copy.start()
            copies.append(copy)
        sent.extend(copies)
        means, moments = [mean], moment
        for offset in range(1, tp):
            copies[offset - 1].wait_recv()
            tile = recv_ref[offset]
            means.append(tile[:, 0:1])
            moments = moments + tile[:, 1:2]
        total = sum(means) * (1.0 / tp)
        for m in means:
            moments = moments + cols * (m - total) * (m - total)
        return (values - total) * lax.rsqrt(moments * (1.0 / (cols * tp)) + norm_eps) * gain[...]

    normed = layer_norm(resid, p2s, p2r, 1, norm1_gain).astype(BF16)

    p3s[...] = dot(place, normed).astype(BF16).reshape(ep, rd, cols)
    routed_copies = []
    for offset in range(1, ep):
        target = ep_peer(offset)
        copy = ep_copy(p3s.at[target], p3r.at[offset], 0, offset, target)
        copy.start()
        routed_copies.append(copy)
    sent.extend(routed_copies)
    p3r[0] = p3s[me_e]

    def send_rows(send_ref, recv_ref, kind, group):
        @pl.when(me_t != group)
        def _():
            pltpu.make_async_remote_copy(
                src_ref=send_ref.at[group],
                dst_ref=recv_ref.at[me_t],
                send_sem=tp_send.at[kind, group],
                recv_sem=tp_recv.at[kind, me_t],
                device_id=(me_e, group),
                device_id_type=pl.DeviceIdType.MESH,
            ).start()

    def settle_sends(send_ref, recv_ref, kind):
        for group in range(groups):

            @pl.when(me_t != group)
            def _():
                tp_copy(send_ref.at[group], recv_ref.at[me_t], kind, group, group).wait_send()

    ready(i_sg)
    ready(i_su)
    shared_gate, shared_up = dot(normed, sg[...]), dot(normed, su[...])
    for group in range(groups):
        part = slice(group * fsc, (group + 1) * fsc)
        p4hs[group, :, 0:fsc] = shared_gate[:, part].astype(BF16)
        p4hs[group, :, fsc : 2 * fsc] = shared_up[:, part].astype(BF16)
        send_rows(p4hs, p4hr, 3, group)

    ready(i_eg)
    ready(i_eu)
    for copy in routed_copies:
        copy.wait_recv()
    incoming = p3r[...].reshape(slots, cols)
    masked = [jnp.where(row_expert == e, incoming, jnp.zeros_like(incoming)) for e in range(local)]
    for group in range(groups):
        part = slice(group * fc, (group + 1) * fc)
        gate_sum = sum(dot(masked[e], eg[e, :, part]) for e in range(local))
        up_sum = sum(dot(masked[e], eu[e, :, part]) for e in range(local))
        p4s[group, :, 0:fc] = gate_sum.astype(BF16)
        p4s[group, :, fc : 2 * fc] = up_sum.astype(BF16)
        send_rows(p4s, p4r, 2, group)

    def reduce(send_ref, recv_ref, kind, dest, kind_out, chunk):
        total = send_ref[me_t].astype(F32)
        for offset in range(1, tp):
            source = tp_peer(offset)
            tp_copy(send_ref.at[0], recv_ref.at[source], kind, source, source).wait_recv()
            total = total + recv_ref[source].astype(F32)
        dest[me_t] = (silu(total[:, 0:chunk]) * total[:, chunk : 2 * chunk]).astype(BF16)
        for offset in range(1, tp):
            pltpu.make_async_remote_copy(
                src_ref=dest.at[me_t],
                dst_ref=dest.at[me_t],
                send_sem=tp_send.at[kind_out, offset],
                recv_sem=tp_recv.at[kind_out, me_t],
                device_id=(me_e, tp_peer(offset)),
                device_id_type=pl.DeviceIdType.MESH,
            ).start()

    def all_reduce():
        reduce(p4hs, p4hr, 3, p5h, 5, fsc)
        reduce(p4s, p4r, 2, p5, 4, fc)

    def gathered(dest, kind):
        for group in range(groups):

            @pl.when(me_t != group)
            def _():
                tp_copy(dest.at[group], dest.at[group], kind, group, group).wait_recv()

    if groups == tp:
        all_reduce()
    else:
        pl.when(me_t < groups)(all_reduce)
    settle_sends(p4hs, p4hr, 3)
    settle_sends(p4s, p4r, 2)
    gathered(p5h, 5)
    ready(i_sd)
    mixture = sum(
        dot(p5h[group], sd[group * fsc : (group + 1) * fsc, :]) for group in range(groups)
    )
    ready(i_ed)
    gathered(p5, 4)
    answer = jnp.zeros((slots, cols), F32)
    for group in range(groups):
        inner = p5[group]
        for e in range(local):
            answer = answer + dot(
                jnp.where(row_expert == e, inner, jnp.zeros_like(inner)),
                ed[e, group * fc : (group + 1) * fc, :],
            )
    p6s[...] = answer.astype(BF16).reshape(ep, rd, cols)
    back_copies = []
    for offset in range(1, ep):
        source = ep_peer(ep - offset)
        copy = ep_copy(p6s.at[offset], p6r.at[ep_peer(0)], 1, offset, source)
        copy.start()
        back_copies.append(copy)
    sent.extend(back_copies)
    p6r[me_e] = p6s[0]
    for offset in range(1, ep):
        expert_dev = ep_peer(offset)
        ep_copy(p6s.at[offset], p6r.at[expert_dev], 1, offset, expert_dev).wait_recv()
    returned = p6r[...].reshape(slots, cols)
    mixture = mixture + dot(gather_hi, returned) + dot(gather_lo, returned)
    last = res_scale * normed.astype(F32) + mixture
    out[...] = layer_norm(last, p7s, p7r, 6, norm2_gain).astype(BF16)
    for copy in sent:
        copy.wait_send()

    def settle_gather(dest, kind):
        for offset in range(1, tp):
            tp_copy(dest.at[me_t], dest.at[me_t], kind, offset, tp_peer(offset)).wait_send()

    def settle_gathers():
        settle_gather(p5, 4)
        settle_gather(p5h, 5)

    if groups == tp:
        settle_gathers()
    else:
        pl.when(me_t < groups)(settle_gathers)


def per_device(
    tokens,
    state,
    w_query,
    w_key,
    w_value,
    w_outgate,
    decay_down,
    decay_up,
    decay_bias,
    head_gain,
    w_output,
    norm1_gain,
    route_ids,
    route_weight,
    exp_gate,
    exp_up,
    exp_down,
    sh_gate,
    sh_up,
    sh_down,
    norm2_gain,
):
    rows, width = tokens.shape
    heads, kdim, vdim = state.shape[1:]
    tp, ep = lax.axis_size("tp"), lax.axis_size("ep")
    cols = width // tp
    top = route_ids.shape[1]
    local = exp_gate.shape[0]
    cap = max(2, rows * top // (local * ep) + 1)
    rd = -(-local * cap // 8) * 8
    slots = ep * rd
    ff, fs = exp_gate.shape[2], sh_gate.shape[1]
    groups = min(tp, ff // 128, fs // 128)
    fc, fsc = ff // groups, fs // groups
    chunks = 4
    dims = (rows, heads, kdim, vdim, cols, tp, ep, local, cap, rd, groups, fc, fsc, top, chunks)
    n_loads = 2 + chunks + 4 + tp + 6
    vm = pltpu.VMEM
    vmem = pl.BlockSpec(memory_space=pltpu.VMEM)
    hbm = pl.BlockSpec(memory_space=pl.ANY)
    return pl.pallas_call(
        functools.partial(kernel, dims),
        out_shape=jax.ShapeDtypeStruct((rows, cols), BF16),
        in_specs=[vmem] * 9 + [hbm] * 12,
        out_specs=vmem,
        scratch_shapes=[
            vm(state.shape, F32),
            vm(w_query.shape, BF16),
            vm(w_key.shape, BF16),
            vm(w_value.shape, BF16),
            vm(w_outgate.shape, BF16),
            vm((tp, w_output.shape[0], cols), BF16),
            vm(exp_gate.shape, BF16),
            vm(exp_up.shape, BF16),
            vm(exp_down.shape, BF16),
            vm(sh_gate.shape, BF16),
            vm(sh_up.shape, BF16),
            vm(sh_down.shape, BF16),
            vm((rows, heads * kdim), F32),
            vm((rows, -(-heads // 8) * 8, vdim), F32),
            vm((rows, heads * vdim), BF16),
            vm((tp, rows, cols), BF16),
            vm((tp, rows, cols), BF16),
            vm((rows, 128), F32),
            vm((tp, rows, 128), F32),
            vm((ep, rd, cols), BF16),
            vm((ep, rd, cols), BF16),
            vm((groups, slots, 2 * fc), BF16),
            vm((tp, slots, 2 * fc), BF16),
            vm((groups, rows, 2 * fsc), BF16),
            vm((tp, rows, 2 * fsc), BF16),
            vm((groups, slots, fc), BF16),
            vm((groups, rows, fsc), BF16),
            vm((ep, rd, cols), BF16),
            vm((ep, rd, cols), BF16),
            vm((rows, 128), F32),
            vm((tp, rows, 128), F32),
            pltpu.SemaphoreType.DMA((n_loads,)),
            pltpu.SemaphoreType.DMA((7, tp)),
            pltpu.SemaphoreType.DMA((7, tp)),
            pltpu.SemaphoreType.DMA((2, ep)),
            pltpu.SemaphoreType.DMA((2, ep)),
        ],
        compiler_params=pltpu.CompilerParams(
            collective_id=0, has_side_effects=True, vmem_limit_bytes=60 * 1024 * 1024
        ),
        name="layer",
    )(
        tokens,
        decay_down,
        decay_up,
        decay_bias[None, :],
        head_gain[None, :],
        norm1_gain[None, :],
        route_ids,
        route_weight,
        norm2_gain[None, :],
        state,
        w_query,
        w_key,
        w_value,
        w_outgate,
        w_output,
        exp_gate,
        exp_up,
        exp_down,
        sh_gate,
        sh_up,
        sh_down,
    )


def solution(mesh):
    in_specs = (
        P("ep", None),
        P("ep", "tp", None, None),
        P(None, "tp"),
        P(None, "tp"),
        P(None, "tp"),
        P(None, "tp"),
        P(),
        P(None, "tp"),
        P("tp"),
        P(),
        P("tp", None),
        P("tp"),
        P("ep", None),
        P("ep", None),
        P("ep", "tp", None),
        P("ep", "tp", None),
        P("ep", None, "tp"),
        P("tp", None),
        P("tp", None),
        P(None, "tp"),
        P("tp"),
    )
    out_specs = P("ep", "tp")
    return jax.shard_map(
        per_device, mesh=mesh, in_specs=in_specs, out_specs=out_specs, check_vma=False
    )
```

```python
import functools

import jax
import jax.numpy as jnp
from jax import lax
from jax.experimental import pallas as pl
from jax.experimental.pallas import tpu as pltpu
from jax.sharding import PartitionSpec as P

res_scale = 2.0**0.5
decay_tau = 16.0
norm_eps = 1e-05
AHEAD = 10
F32 = jnp.float32
BF16 = jnp.bfloat16


def dot(left, right):
    return jnp.dot(left, right, preferred_element_type=F32)


def dot_nt(left, right):
    return lax.dot_general(left, right, (((1,), (1,)), ((), ())), preferred_element_type=F32)


def iota_f(shape, dim):
    return lax.broadcasted_iota(jnp.int32, shape, dim).astype(F32)


def quotient(values, divisor):
    return jnp.floor((values + 0.5) * (1.0 / divisor))


def silu(x):
    return x * (1.0 / (1.0 + jnp.exp(-x)))


def kernel(
    dims,
    tokens,
    decay_down,
    decay_up,
    decay_bias,
    head_gain,
    norm1_gain,
    route_ids,
    route_weight,
    norm2_gain,
    state_h,
    wq_h,
    wk_h,
    wv_h,
    wg_h,
    wo_h,
    eg_h,
    eu_h,
    ed_h,
    sg_h,
    su_h,
    sd_h,
    out,
    state,
    wq,
    wk,
    wv,
    wg,
    wo,
    eg,
    eu,
    ed,
    sg,
    su,
    sd,
    dq_ref,
    att_ref,
    head_out,
    p1s,
    p1r,
    p2s,
    p2r,
    p3s,
    p3r,
    p4s,
    p4r,
    p4hs,
    p4hr,
    p5,
    p5h,
    p6s,
    p6r,
    p7s,
    p7r,
    load_sem,
    tp_send,
    tp_recv,
    ep_send,
    ep_recv,
):
    (rows, heads, kdim, vdim, cols, tp, ep, local, cap, rd, groups, fc, fsc, top, chunks) = dims
    experts = local * ep
    slots = ep * rd
    me_t = lax.axis_index("tp")
    me_e = lax.axis_index("ep")

    def tp_peer(offset):
        return lax.rem(me_t + offset, tp)

    def ep_peer(offset):
        return lax.rem(me_e + offset, ep)

    barrier = pltpu.get_barrier_semaphore()
    for offset in range(1, tp):
        pl.semaphore_signal(
            barrier, inc=1, device_id=(me_e, tp_peer(offset)), device_id_type=pl.DeviceIdType.MESH
        )
    for offset in range(1, ep):
        pl.semaphore_signal(
            barrier, inc=1, device_id=(ep_peer(offset), me_t), device_id_type=pl.DeviceIdType.MESH
        )

    loads = []

    def add_load(src, dst):
        loads.append(pltpu.make_async_copy(src, dst, load_sem.at[len(loads)]))
        return len(loads) - 1

    step = rows // chunks
    i_wq = add_load(wq_h, wq)
    i_wk = add_load(wk_h, wk)
    i_state = [
        add_load(state_h.at[pl.ds(c * step, step)], state.at[pl.ds(c * step, step)])
        for c in range(chunks)
    ]
    half = wv_h.shape[0] // 2
    i_wv = [add_load(wv_h.at[pl.ds(c * half, half)], wv.at[pl.ds(c * half, half)]) for c in range(2)]
    i_wg = [add_load(wg_h.at[pl.ds(c * half, half)], wg.at[pl.ds(c * half, half)]) for c in range(2)]
    i_wo = []
    for offset in range(tp):
        start = pl.multiple_of(tp_peer(offset + 1) * cols, 128)
        i_wo.append(add_load(wo_h.at[:, pl.ds(start, cols)], wo.at[offset]))
    i_sg = add_load(sg_h, sg)
    i_su = add_load(su_h, su)
    i_eg = add_load(eg_h, eg)
    i_eu = add_load(eu_h, eu)
    i_sd = add_load(sd_h, sd)
    i_ed = add_load(ed_h, ed)
    for copy in loads[:AHEAD]:
        copy.start()

    def ready(index):
        loads[index].wait()
        if index + AHEAD < len(loads):
            loads[index + AHEAD].start()

    def tp_copy(src, dst, kind, slot, target):
        return pltpu.make_async_remote_copy(
            src_ref=src,
            dst_ref=dst,
            send_sem=tp_send.at[kind, slot],
            recv_sem=tp_recv.at[kind, slot],
            device_id=(me_e, target),
            device_id_type=pl.DeviceIdType.MESH,
        )

    def ep_copy(src, dst, kind, slot, target):
        return pltpu.make_async_remote_copy(
            src_ref=src,
            dst_ref=dst,
            send_sem=ep_send.at[kind, slot],
            recv_sem=ep_recv.at[kind, slot],
            device_id=(target, me_t),
            device_id_type=pl.DeviceIdType.MESH,
        )

    tok = tokens[...]
    decay_low = dot_nt(tok, decay_down[...]).astype(BF16)
    pre = dot(decay_low, decay_up[...]) + decay_bias[...]
    log_decay = (jnp.minimum(pre, 0.0) - jnp.log(1.0 + jnp.exp(-jnp.abs(pre)))) * (1.0 / decay_tau)
    ids = route_ids[...]
    weights = route_weight[...]
    expert_iota = lax.broadcasted_iota(jnp.int32, (experts, rows), 0)
    member = jnp.zeros((experts, rows), F32)
    weight_of = jnp.zeros((experts, rows), F32)
    for k in range(top):
        hit = ids[k : k + 1, :] == expert_iota
        member = jnp.where(hit, 1.0, member)
        weight_of = jnp.where(hit, weights[k : k + 1, :], weight_of)
    member_b = member.astype(BF16)
    earlier = (iota_f((rows, rows), 0) < iota_f((rows, rows), 1)).astype(F32).astype(BF16)
    identity = (iota_f((rows, rows), 0) == iota_f((rows, rows), 1)).astype(F32).astype(BF16)
    rank_b = dot(member_b, earlier).astype(BF16)

    def slot_parts(number):
        dest = quotient(number, rd)
        inner = number - dest * rd
        which = quotient(inner, cap)
        return dest * local + which, inner - which * cap, which, inner < local * cap

    e_col, c_col, _, ok_col = slot_parts(iota_f((slots, 1), 0))
    expand = ((iota_f((slots, experts), 1) == e_col) & ok_col).astype(F32).astype(BF16)
    placed = (dot(expand, member_b) > 0.5) & (dot(expand, rank_b) == c_col)
    place = jnp.where(placed, 1.0, 0.0).astype(BF16)
    weight_hi = weight_of.astype(BF16)
    weight_lo = (weight_of - weight_hi.astype(F32)).astype(BF16)
    spread_hi = jnp.where(placed, dot(expand, weight_hi), 0.0).astype(BF16)
    spread_lo = jnp.where(placed, dot(expand, weight_lo), 0.0).astype(BF16)
    per = ep * cap
    packed = local * per

    def packed_slot(number):
        which = quotient(number, per)
        inner = number - which * per
        source = quotient(inner, cap)
        return source * rd + which * cap + inner - source * cap

    squeeze = packed_slot(iota_f((packed, slots), 0)) == iota_f((packed, slots), 1)
    squeeze = jnp.where(squeeze, 1.0, 0.0).astype(BF16)
    widen = packed_slot(iota_f((slots, packed), 1)) == iota_f((slots, packed), 0)
    widen = jnp.where(widen, 1.0, 0.0).astype(BF16)
    gather_hi = dot_nt(identity, spread_hi).astype(BF16)
    gather_lo = dot_nt(identity, spread_lo).astype(BF16)

    ready(i_wq)
    queries = dot(tok, wq[...]).astype(BF16).astype(F32) * kdim ** (-0.5)
    dq_ref[...] = queries * jnp.exp(log_decay)
    ready(i_wk)
    key_rows = dot(tok, wk[...]).astype(BF16).astype(F32)
    pairs = queries * key_rows
    width = heads * kdim
    hr = att_ref.shape[1]
    head_mask = quotient(iota_f((hr, width), 1), kdim) == iota_f((hr, width), 0)
    for c in range(chunks):
        ready(i_state[c])

        def one_row(b, carry):
            left = jnp.where(head_mask, dq_ref[pl.ds(b, 1), :], 0.0).astype(BF16)
            right = state[b].reshape(width, vdim).astype(BF16)
            att_ref[b] = dot(left, right)
            return carry

        lax.fori_loop(c * step, (c + 1) * step, one_row, 0, unroll=min(step, 3))
    for i in i_wv:
        ready(i)
    values = dot(tok, wv[...]).astype(BF16).astype(F32)
    for i in i_wg:
        ready(i)
    gate_pre = dot(tok, wg[...]).astype(BF16).astype(F32)
    for h in range(heads):
        part = slice(h * vdim, (h + 1) * vdim)
        score = jnp.sum(pairs[:, h * kdim : (h + 1) * kdim], -1, keepdims=True)
        attended = att_ref[:, h, :] + score * values[:, part]
        inv = lax.rsqrt(jnp.mean(attended * attended, -1, keepdims=True) + norm_eps)
        head_out[:, part] = (attended * inv * head_gain[...] * silu(gate_pre[:, part])).astype(BF16)
    pl.semaphore_wait(barrier, tp - 1 + ep - 1)

    sent = []
    heads_side = head_out[...]
    own = None
    for offset in range(1, tp + 1):
        ready(i_wo[offset - 1])
        product = dot(heads_side, wo[offset - 1])
        if offset < tp:
            p1s[offset] = product.astype(BF16)
            copy = tp_copy(p1s.at[offset], p1r.at[offset], 0, offset, tp_peer(offset))
            copy.start()
            sent.append(copy)
        else:
            own = product
    start = pl.multiple_of(me_t * cols, 128)
    resid = own + res_scale * tokens[:, pl.ds(start, cols)].astype(F32)
    for offset in range(1, tp):
        sent[offset - 1].wait_recv()
        resid = resid + p1r[offset].astype(F32)

    def layer_norm(values, send_ref, recv_ref, kind, gain):
        mean = jnp.mean(values, -1, keepdims=True)
        center = values - mean
        moment = jnp.sum(center * center, -1, keepdims=True)
        lane = lax.broadcasted_iota(jnp.int32, (rows, 128), 1)
        send_ref[...] = jnp.where(lane == 0, mean, moment)
        copies = []
        for offset in range(1, tp):
            copy = tp_copy(send_ref, recv_ref.at[offset], kind, offset, tp_peer(offset))
            copy.start()
            copies.append(copy)
        sent.extend(copies)
        means, moments = [mean], moment
        for offset in range(1, tp):
            copies[offset - 1].wait_recv()
            tile = recv_ref[offset]
            means.append(tile[:, 0:1])
            moments = moments + tile[:, 1:2]
        total = sum(means) * (1.0 / tp)
        for m in means:
            moments = moments + cols * (m - total) * (m - total)
        return (values - total) * lax.rsqrt(moments * (1.0 / (cols * tp)) + norm_eps) * gain[...]

    normed = layer_norm(resid, p2s, p2r, 1, norm1_gain).astype(BF16)

    p3s[...] = dot(place, normed).astype(BF16).reshape(ep, rd, cols)
    routed_copies = []
    for offset in sorted(range(1, ep), key=lambda o: -min(o, ep - o)):
        target = ep_peer(offset)
        copy = ep_copy(p3s.at[target], p3r.at[offset], 0, offset, target)
        copy.start()
        routed_copies.append(copy)
    sent.extend(routed_copies)
    p3r[0] = p3s[me_e]

    def send_rows(send_ref, recv_ref, kind, group):
        @pl.when(me_t != group)
        def _():
            pltpu.make_async_remote_copy(
                src_ref=send_ref.at[group],
                dst_ref=recv_ref.at[me_t],
                send_sem=tp_send.at[kind, group],
                recv_sem=tp_recv.at[kind, me_t],
                device_id=(me_e, group),
                device_id_type=pl.DeviceIdType.MESH,
            ).start()

    def settle_sends(send_ref, recv_ref, kind):
        for group in range(groups):

            @pl.when(me_t != group)
            def _():
                tp_copy(send_ref.at[group], recv_ref.at[me_t], kind, group, group).wait_send()

    ready(i_sg)
    ready(i_su)
    shared_gate, shared_up = dot(normed, sg[...]), dot(normed, su[...])
    for group in range(groups):
        part = slice(group * fsc, (group + 1) * fsc)
        p4hs[group, :, 0:fsc] = shared_gate[:, part].astype(BF16)
        p4hs[group, :, fsc : 2 * fsc] = shared_up[:, part].astype(BF16)
        send_rows(p4hs, p4hr, 3, group)

    ready(i_eg)
    ready(i_eu)
    for copy in routed_copies:
        copy.wait_recv()
    incoming = dot(squeeze, p3r[...].reshape(slots, cols))
    chosen = [incoming[e * per : (e + 1) * per].astype(BF16) for e in range(local)]
    slab = 2 if groups % 2 == 0 else 1
    for first in range(0, groups, slab):
        part = slice(first * fc, (first + slab) * fc)
        for e in range(local):
            at = slice(e * per, (e + 1) * per)
            gate_sum = dot(chosen[e], eg[e, :, part])
            up_sum = dot(chosen[e], eu[e, :, part])
            for i in range(slab):
                cut = slice(i * fc, (i + 1) * fc)
                p4s[first + i, at, 0:fc] = gate_sum[:, cut].astype(BF16)
                p4s[first + i, at, fc : 2 * fc] = up_sum[:, cut].astype(BF16)
        for i in range(slab):
            send_rows(p4s, p4r, 2, first + i)

    def reduce(send_ref, recv_ref, kind, dest, kind_out, chunk):
        total = send_ref[me_t].astype(F32)
        for offset in range(1, tp):
            source = tp_peer(offset)
            tp_copy(send_ref.at[0], recv_ref.at[source], kind, source, source).wait_recv()
            total = total + recv_ref[source].astype(F32)
        dest[me_t] = (silu(total[:, 0:chunk]) * total[:, chunk : 2 * chunk]).astype(BF16)
        for offset in range(1, tp):
            pltpu.make_async_remote_copy(
                src_ref=dest.at[me_t],
                dst_ref=dest.at[me_t],
                send_sem=tp_send.at[kind_out, offset],
                recv_sem=tp_recv.at[kind_out, me_t],
                device_id=(me_e, tp_peer(offset)),
                device_id_type=pl.DeviceIdType.MESH,
            ).start()

    def all_reduce():
        reduce(p4hs, p4hr, 3, p5h, 5, fsc)
        reduce(p4s, p4r, 2, p5, 4, fc)

    def gathered(dest, kind):
        for group in range(groups):

            @pl.when(me_t != group)
            def _():
                tp_copy(dest.at[group], dest.at[group], kind, group, group).wait_recv()

    if groups == tp:
        all_reduce()
    else:
        pl.when(me_t < groups)(all_reduce)
    settle_sends(p4hs, p4hr, 3)
    settle_sends(p4s, p4r, 2)
    gathered(p5h, 5)
    ready(i_sd)
    mixture = sum(
        dot(p5h[group], sd[group * fsc : (group + 1) * fsc, :]) for group in range(groups)
    )
    ready(i_ed)
    gathered(p5, 4)
    inner = jnp.concatenate([p5[group] for group in range(groups)], 1).astype(F32)
    answer = jnp.concatenate(
        [dot(inner[e * per : (e + 1) * per].astype(BF16), ed[e]) for e in range(local)], 0
    ).astype(BF16)
    p6s[...] = dot(widen, answer).astype(BF16).reshape(ep, rd, cols)
    back_copies = []
    for offset in sorted(range(1, ep), key=lambda o: -min(o, ep - o)):
        source = ep_peer(ep - offset)
        copy = ep_copy(p6s.at[offset], p6r.at[ep_peer(0)], 1, offset, source)
        copy.start()
        back_copies.append(copy)
    sent.extend(back_copies)
    p6r[me_e] = p6s[0]
    for offset in range(1, ep):
        expert_dev = ep_peer(offset)
        ep_copy(p6s.at[offset], p6r.at[expert_dev], 1, offset, expert_dev).wait_recv()
    returned = p6r[...].reshape(slots, cols)
    mixture = mixture + dot(gather_hi, returned) + dot(gather_lo, returned)
    last = res_scale * normed.astype(F32) + mixture
    out[...] = layer_norm(last, p7s, p7r, 6, norm2_gain).astype(BF16)
    for copy in sent:
        copy.wait_send()

    def settle_gather(dest, kind):
        for offset in range(1, tp):
            tp_copy(dest.at[me_t], dest.at[me_t], kind, offset, tp_peer(offset)).wait_send()

    def settle_gathers():
        settle_gather(p5, 4)
        settle_gather(p5h, 5)

    if groups == tp:
        settle_gathers()
    else:
        pl.when(me_t < groups)(settle_gathers)


def per_device(
    tokens,
    state,
    w_query,
    w_key,
    w_value,
    w_outgate,
    decay_down,
    decay_up,
    decay_bias,
    head_gain,
    w_output,
    norm1_gain,
    route_ids,
    route_weight,
    exp_gate,
    exp_up,
    exp_down,
    sh_gate,
    sh_up,
    sh_down,
    norm2_gain,
):
    rows, width = tokens.shape
    heads, kdim, vdim = state.shape[1:]
    tp, ep = lax.axis_size("tp"), lax.axis_size("ep")
    cols = width // tp
    top = route_ids.shape[1]
    local = exp_gate.shape[0]
    cap = max(2, rows * top // (local * ep) + 1)
    rd = -(-local * cap // 8) * 8
    packed = local * cap * ep
    ff, fs = exp_gate.shape[2], sh_gate.shape[1]
    groups = min(tp, ff // 128, fs // 128)
    fc, fsc = ff // groups, fs // groups
    chunks = 4
    dims = (rows, heads, kdim, vdim, cols, tp, ep, local, cap, rd, groups, fc, fsc, top, chunks)
    n_loads = 2 + chunks + 4 + tp + 6
    vm = pltpu.VMEM
    vmem = pl.BlockSpec(memory_space=pltpu.VMEM)
    hbm = pl.BlockSpec(memory_space=pl.ANY)
    return pl.pallas_call(
        functools.partial(kernel, dims),
        out_shape=jax.ShapeDtypeStruct((rows, cols), BF16),
        in_specs=[vmem] * 9 + [hbm] * 12,
        out_specs=vmem,
        scratch_shapes=[
            vm(state.shape, F32),
            vm(w_query.shape, BF16),
            vm(w_key.shape, BF16),
            vm(w_value.shape, BF16),
            vm(w_outgate.shape, BF16),
            vm((tp, w_output.shape[0], cols), BF16),
            vm(exp_gate.shape, BF16),
            vm(exp_up.shape, BF16),
            vm(exp_down.shape, BF16),
            vm(sh_gate.shape, BF16),
            vm(sh_up.shape, BF16),
            vm(sh_down.shape, BF16),
            vm((rows, heads * kdim), F32),
            vm((rows, -(-heads // 8) * 8, vdim), F32),
            vm((rows, heads * vdim), BF16),
            vm((tp, rows, cols), BF16),
            vm((tp, rows, cols), BF16),
            vm((rows, 128), F32),
            vm((tp, rows, 128), F32),
            vm((ep, rd, cols), BF16),
            vm((ep, rd, cols), BF16),
            vm((groups, packed, 2 * fc), BF16),
            vm((tp, packed, 2 * fc), BF16),
            vm((groups, rows, 2 * fsc), BF16),
            vm((tp, rows, 2 * fsc), BF16),
            vm((groups, packed, fc), BF16),
            vm((groups, rows, fsc), BF16),
            vm((ep, rd, cols), BF16),
            vm((ep, rd, cols), BF16),
            vm((rows, 128), F32),
            vm((tp, rows, 128), F32),
            pltpu.SemaphoreType.DMA((n_loads,)),
            pltpu.SemaphoreType.DMA((7, tp)),
            pltpu.SemaphoreType.DMA((7, tp)),
            pltpu.SemaphoreType.DMA((2, ep)),
            pltpu.SemaphoreType.DMA((2, ep)),
        ],
        compiler_params=pltpu.CompilerParams(
            collective_id=0, has_side_effects=True, vmem_limit_bytes=60 * 1024 * 1024
        ),
        name="layer",
    )(
        tokens,
        decay_down.T,
        decay_up,
        decay_bias[None, :],
        head_gain[None, :],
        norm1_gain[None, :],
        route_ids.T,
        route_weight.T,
        norm2_gain[None, :],
        state,
        w_query,
        w_key,
        w_value,
        w_outgate,
        w_output,
        exp_gate,
        exp_up,
        exp_down,
        sh_gate,
        sh_up,
        sh_down,
    )


def solution(mesh):
    in_specs = (
        P("ep", None),
        P("ep", "tp", None, None),
        P(None, "tp"),
        P(None, "tp"),
        P(None, "tp"),
        P(None, "tp"),
        P(),
        P(None, "tp"),
        P("tp"),
        P(),
        P("tp", None),
        P("tp"),
        P("ep", None),
        P("ep", None),
        P("ep", "tp", None),
        P("ep", "tp", None),
        P("ep", None, "tp"),
        P("tp", None),
        P("tp", None),
        P(None, "tp"),
        P("tp"),
    )
    out_specs = P("ep", "tp")
    return jax.shard_map(
        per_device, mesh=mesh, in_specs=in_specs, out_specs=out_specs, check_vma=False
    )
```
